32 devices in a mesh: sp: 4 (over z), tp: 8 (over y, x, core).
Axes of the slice: x: 2, y: 2, z: 4, core: 2. Of those that a mesh axis runs over, the one named last changes fastest.
Arguments:
- latent: bfloat16 [1024, 4096], P(('sp', 'tp')), may hold values from -16 to 16
- context: bfloat16 [256, 4096], P('sp'), may hold values from -16 to 16
- cond: bfloat16 [4096], P('sp'), may hold values from -6 to 6
- cond_ctx: bfloat16 [4096], P('sp'), may hold values from -6 to 6
- mod_shift_w: bfloat16 [4096, 4096], P('sp', 'tp'), may hold values from -0.15625 to 0.15625
- mod_scale_w: bfloat16 [4096, 4096], P('sp', 'tp'), may hold values from -0.15625 to 0.15625
- mod_gate_w: bfloat16 [4096, 4096], P('sp', 'tp'), may hold values from -0.15625 to 0.15625
- norm_gain: bfloat16 [4096], replicated, may hold values from 0.099609375 to 1.8984375
- proj_z: bfloat16 [4096, 4096], P(None, 'tp'), may hold values from -0.09375 to 0.09375
- proj_x: bfloat16 [4096, 4096], P(None, 'tp'), may hold values from -0.09375 to 0.09375
- proj_b: bfloat16 [4096, 8192], P(None, 'tp'), may hold values from -0.09375 to 0.09375
- proj_c: bfloat16 [4096, 8192], P(None, 'tp'), may hold values from -0.09375 to 0.09375
- proj_dt: bfloat16 [4096, 128], replicated, may hold values from -0.09375 to 0.09375
- conv_x: bfloat16 [3, 4096], P(None, 'tp'), may hold values from -3.5 to 3.5
- conv_b: bfloat16 [3, 8192], P(None, 'tp'), may hold values from -3.5 to 3.5
- conv_c: bfloat16 [3, 8192], P(None, 'tp'), may hold values from -3.5 to 3.5
- dt_bias: float32 [128], P('tp'), may hold values from -1 to 1
- decay_log: float32 [128], P('tp'), may hold values from -11.6 to -2.9
- head_gain: bfloat16 [4096], P('tp'), may hold values from 0.099609375 to 1.8984375
- proj_out: bfloat16 [4096, 4096], P(None, 'tp'), may hold values from -0.09375 to 0.09375
Outputs:
- mixed: bfloat16 [1024, 4096], P(('sp', 'tp'))
The draws below stay inside these ranges and needn't reach their ends.
All inputs are finite; a program needn't handle non-finite values.
Results may differ from the reference program's by a relative error of at most 0.0065.
Values may be sent and summed in bfloat16 or wider, within the bound.
A program may use at most 128 MiB of HBM per device.

```python
import jax
import jax.numpy as jnp
from jax import lax

D = 4096
HEADS = 64
HEAD_DIM = 64
STATE = 128
BLOCK = 128
CTX = 256
SEQ = 1024


def draw_latent(key, part):
    key_noise = jax.random.fold_in(key, 11)
    key_dir = jax.random.fold_in(key, 12)
    key_level = jax.random.fold_in(key, 13)
    direction = jax.random.normal(key_dir, (D,), jnp.float32)
    levels = jax.random.uniform(key_level, (SEQ // BLOCK,), jnp.float32, -1.5, 1.5)
    offsets = jnp.repeat(levels, BLOCK, total_repeat_length=SEQ)[:, None] * direction[None, :]
    noise = jax.random.normal(key_noise, (SEQ, D), jnp.float32)
    return jnp.clip(noise + offsets, -16.0, 16.0).astype(jnp.bfloat16)


def draw_context(key, part):
    key_noise = jax.random.fold_in(key, 31)
    key_seg = jax.random.fold_in(key, 32)
    segment = CTX // 16
    directions = jax.random.normal(key_seg, (16, D), jnp.float32) * 4.0
    offsets = jnp.repeat(directions, segment, axis=0, total_repeat_length=CTX)
    noise = jax.random.normal(key_noise, (CTX, D), jnp.float32) * 0.7
    return jnp.clip(noise + offsets, -16.0, 16.0).astype(jnp.bfloat16)


def draw_decay_log(key, part):
    key_pick = jax.random.fold_in(key, 21)
    key_slow = jax.random.fold_in(key, 22)
    key_fast = jax.random.fold_in(key, 23)
    slow = jax.random.uniform(key_slow, (2 * HEADS,), jnp.float32, -11.5, -9.45)
    fast = jax.random.uniform(key_fast, (2 * HEADS,), jnp.float32, -4.2, -3.0)
    share = 0.5
    pick = jax.random.uniform(key_pick, (2 * HEADS,), jnp.float32) < share
    return jnp.where(pick, fast, slow)


def shard_levels(key, dims, shards, least, largest):
    level, own = 1.0, jax.random.fold_in(key, 6)
    for axis_at, blocks in shards:
        draws = jnp.exp(jax.random.uniform(jax.random.fold_in(own, axis_at), (blocks,), jnp.float32, least / len(shards), largest / len(shards)))
        level = level * jnp.repeat(draws, dims[axis_at] // blocks).reshape([-1 if axis == axis_at else 1 for axis in range(len(dims))])
    return level


def scatter_about(rng, shape, deviation, most, split=(), dtype=jnp.bfloat16):
    loudness = shard_levels(rng, shape, split, -0.22, 0.18) if split else 1.0
    array = jax.random.normal(rng, shape, jnp.float32) * deviation * loudness
    return jnp.minimum(jnp.maximum(array, -most), most).astype(dtype)


def setup_inputs(seed: int = 0) -> dict:
    keys = jax.random.split(jax.random.key(seed), 21)
    latent = draw_latent(jax.random.fold_in(keys[20], 71), 0)
    context = draw_context(jax.random.fold_in(keys[20], 71), 0)
    cond = scatter_about(keys[2], (D,), 1.0, 6.0, ((0, 4),))
    cond_ctx = scatter_about(keys[3], (D,), 1.0, 6.0, ((0, 4),))
    mod_shift_w = scatter_about(keys[4], (D, D), (D // 3) ** -0.5, 0.15625, ((0, 4), (1, 8)))
    mod_scale_w = scatter_about(keys[5], (D, D), (D // 3) ** -0.5, 0.15625, ((0, 4), (1, 8)))
    mod_gate_w = scatter_about(keys[6], (D, D), (D // 3) ** -0.5, 0.15625, ((0, 4), (1, 8)))
    norm_gain = jnp.clip(1.0 + 0.18 * jax.random.normal(keys[7], (D,), jnp.float32), 0.099609375, 1.8984375).astype(jnp.bfloat16)
    proj_z = scatter_about(keys[8], (D, D), D ** -0.5, 0.09375, ((1, 8),))
    proj_x = scatter_about(keys[9], (D, D), D ** -0.5, 0.09375, ((1, 8),))
    proj_b = scatter_about(keys[10], (D, HEADS * STATE), D ** -0.5, 0.09375, ((1, 8),))
    proj_c = scatter_about(keys[11], (D, HEADS * STATE), D ** -0.5, 0.09375, ((1, 8),))
    proj_dt = scatter_about(keys[12], (D, 2 * HEADS), D ** -0.5, 0.09375)
    conv_x = scatter_about(keys[13], (3, D), 3 ** -0.5, 3.5, ((1, 8),))
    conv_b = scatter_about(keys[14], (3, HEADS * STATE), 3 ** -0.5, 3.5, ((1, 8),))
    conv_c = scatter_about(keys[15], (3, HEADS * STATE), 3 ** -0.5, 3.5, ((1, 8),))
    dt_bias = jnp.clip(jax.random.uniform(keys[16], (2 * HEADS,), jnp.float32, -1.0, 1.0) * shard_levels(keys[16], (2 * HEADS,), ((0, 8),), -0.4, 0.0), -1.0, 1.0)
    decay_log = draw_decay_log(jax.random.fold_in(keys[20], 71), 0)
    head_gain = jnp.clip(1.0 + 0.18 * jax.random.normal(keys[18], (D,), jnp.float32), 0.099609375, 1.8984375).astype(jnp.bfloat16)
    proj_out = scatter_about(keys[19], (D, D), D ** -0.5, 0.09375, ((1, 8),))
    return dict(latent=latent, context=context, cond=cond, cond_ctx=cond_ctx, mod_shift_w=mod_shift_w, mod_scale_w=mod_scale_w, mod_gate_w=mod_gate_w, norm_gain=norm_gain, proj_z=proj_z, proj_x=proj_x, proj_b=proj_b, proj_c=proj_c, proj_dt=proj_dt, conv_x=conv_x, conv_b=conv_b, conv_c=conv_c, dt_bias=dt_bias, decay_log=decay_log, head_gain=head_gain, proj_out=proj_out)


EPS = 1e-06

def modulated_norm(rows, gain, shift, scale):
    wide = rows.astype(jnp.float32)
    normed = wide * lax.rsqrt(lax.optimization_barrier(jnp.mean(wide * wide, axis=-1, keepdims=True)) + EPS) * gain.astype(jnp.float32)
    return (normed * (1.0 + scale) + shift).astype(jnp.bfloat16)

def project(rows, weights):
    outputs = [jnp.dot(rows, w, preferred_element_type=jnp.float32).astype(jnp.bfloat16) for w in weights]
    return lax.optimization_barrier(outputs)

def centred_conv(padded, taps):
    wide = padded.astype(jnp.float32)
    weights = taps.astype(jnp.float32)
    length = padded.shape[0] - 2
    return jax.nn.silu(weights[0] * wide[:length] + weights[1] * wide[1:length + 1] + weights[2] * wide[2:])

def zero_pad(values):
    return jnp.pad(values, ((1, 1), (0, 0)))

def block_states(values, writes, step_size, decay_rate, block):
    length, heads, width = values.shape
    state = writes.shape[2]
    count = length // block
    log_decay = jnp.cumsum(-(step_size * decay_rate).reshape(count, block, heads), axis=1)
    scaled_values = (values * step_size[:, :, None]).reshape(count, block, heads, width)
    write_blocks = writes.reshape(count, block, heads, state)
    tail = jnp.exp(log_decay[:, -1:] - log_decay)
    block_sums = jnp.einsum('kshn,ksh,kshp->khpn', write_blocks, tail, scaled_values, precision=lax.Precision.HIGHEST)
    block_decay = jnp.exp(log_decay[:, -1])

    def advance(carry, inputs):
        block_sum, decay = inputs
        return (carry * decay[:, None, None] + block_sum, carry)
    final, entering = lax.scan(advance, jnp.zeros((heads, width, state), jnp.float32), (block_sums, block_decay))
    overall = jnp.exp(lax.optimization_barrier(jnp.sum(log_decay[:, -1], axis=0)))
    return (log_decay, scaled_values, entering, final, overall)

def block_outputs(reads, writes, log_decay, scaled_values, entering, start_state):
    count, block, heads = log_decay.shape
    state = reads.shape[2]
    read_blocks = reads.reshape(count, block, heads, state)
    write_blocks = writes.reshape(count, block, heads, state)
    starts = jnp.cumsum(log_decay[:, -1], axis=0) - log_decay[:, -1]
    entering_all = entering + jnp.exp(starts)[:, :, None, None] * start_state[None]
    forward_mask = jnp.tril(jnp.ones((block, block), bool))[None, :, :, None]
    spans = log_decay[:, :, None, :] - log_decay[:, None, :, :]
    weights = jnp.where(forward_mask, jnp.exp(jnp.where(forward_mask, spans, 0.0)), 0.0)
    intersection = jnp.einsum('kqhn,kshn->kqsh', read_blocks, write_blocks, precision=lax.Precision.HIGHEST)
    within = jnp.einsum('kqsh,kshp->kqhp', intersection * weights, scaled_values, precision=lax.Precision.HIGHEST)
    carried = jnp.einsum('kqhn,khpn->kqhp', read_blocks, entering_all, precision=lax.Precision.HIGHEST) * jnp.exp(log_decay)[..., None]
    return (within + carried).reshape(count * block, heads, -1)

def reference(latent, context, cond, cond_ctx, mod_shift_w, mod_scale_w, mod_gate_w, norm_gain, proj_z, proj_x, proj_b, proj_c, proj_dt, conv_x, conv_b, conv_c, dt_bias, decay_log, head_gain, proj_out):
    act = jax.nn.silu(cond.astype(jnp.float32)).astype(jnp.bfloat16)
    act_ctx = jax.nn.silu(cond_ctx.astype(jnp.float32)).astype(jnp.bfloat16)
    shift = jnp.dot(act, mod_shift_w, preferred_element_type=jnp.float32)
    scale = jnp.dot(act, mod_scale_w, preferred_element_type=jnp.float32)
    gate = jnp.dot(act, mod_gate_w, preferred_element_type=jnp.float32)
    ctx_shift = jnp.dot(act_ctx, mod_shift_w, preferred_element_type=jnp.float32)
    ctx_scale = jnp.dot(act_ctx, mod_scale_w, preferred_element_type=jnp.float32)
    normed_rows = modulated_norm(latent, norm_gain, shift, scale)
    normed_ctx = modulated_norm(context, norm_gain, ctx_shift, ctx_scale)
    x_in, b_in, c_in, z_in, dt_raw = project(normed_rows, (proj_x, proj_b, proj_c, proj_z, proj_dt))
    x_ctx, b_ctx, dt_ctx = project(normed_ctx, (proj_x, proj_b, proj_dt))
    values = centred_conv(zero_pad(x_in), conv_x).reshape(SEQ, HEADS, HEAD_DIM)
    writes = centred_conv(zero_pad(b_in), conv_b).reshape(SEQ, HEADS, STATE)
    reads = centred_conv(zero_pad(c_in), conv_c).reshape(SEQ, HEADS, STATE)
    values_ctx = centred_conv(zero_pad(x_ctx), conv_x).reshape(CTX, HEADS, HEAD_DIM)
    writes_ctx = centred_conv(zero_pad(b_ctx), conv_b).reshape(CTX, HEADS, STATE)
    step_size = jax.nn.softplus(dt_raw.astype(jnp.float32) + dt_bias).reshape(SEQ, HEADS, 2)
    step_ctx = jax.nn.softplus(dt_ctx.astype(jnp.float32) + dt_bias).reshape(CTX, HEADS, 2)
    decay_rate = jnp.exp(decay_log).reshape(HEADS, 2)
    ctx_f = block_states(values_ctx, writes_ctx, step_ctx[:, :, 0], decay_rate[:, 0], BLOCK)[3]
    ctx_b = block_states(jnp.flip(values_ctx, 0), jnp.flip(writes_ctx, 0), jnp.flip(step_ctx[:, :, 1], 0), decay_rate[:, 1], BLOCK)[3]
    log_f, scaled_f, enter_f, _, _ = block_states(values, writes, step_size[:, :, 0], decay_rate[:, 0], BLOCK)
    out_f = block_outputs(reads, writes, log_f, scaled_f, enter_f, ctx_f)
    log_b, scaled_b, enter_b, _, _ = block_states(jnp.flip(values, 0), jnp.flip(writes, 0), jnp.flip(step_size[:, :, 1], 0), decay_rate[:, 1], BLOCK)
    out_b = block_outputs(jnp.flip(reads, 0), jnp.flip(writes, 0), log_b, scaled_b, enter_b, ctx_b)
    summed = out_f + jnp.flip(out_b, 0)
    gated = summed * jax.nn.silu(z_in.astype(jnp.float32)).reshape(SEQ, HEADS, HEAD_DIM)
    gated = gated * lax.rsqrt(lax.optimization_barrier(jnp.mean(gated * gated, axis=-1, keepdims=True)) + EPS)
    gated = gated * head_gain.astype(jnp.float32).reshape(HEADS, HEAD_DIM)
    mixed_heads = gated.reshape(SEQ, D).astype(jnp.bfloat16)
    update = jnp.dot(mixed_heads, proj_out, preferred_element_type=jnp.float32).astype(jnp.bfloat16)
    update = lax.optimization_barrier(update).astype(jnp.float32)
    return (latent.astype(jnp.float32) + gate * update).astype(jnp.bfloat16)
```

```python
import functools

import jax
import jax.numpy as jnp
from jax import lax
from jax.experimental import pallas as pl
from jax.experimental.pallas import tpu as pltpu
from jax.sharding import PartitionSpec as P

HEAD_DIM = 64
BLOCK = 128


EPS = 1e-06


def extended(array, sides, width):
    for axis, dim in sides:
        count, length = (lax.axis_size(axis), array.shape[dim])
        up = [(i, (i + 1) % count) for i in range(count - 1)]
        down = [(j, i) for i, j in up]
        last = lax.slice_in_dim(array, length - width, length, axis=dim)
        first = lax.slice_in_dim(array, 0, width, axis=dim)
        before = lax.ppermute(last, axis, up)
        after = lax.ppermute(first, axis, down)
        array = jnp.concatenate([before, array, after], axis=dim)
    return array


def entering_2(array, axis, combine, identity, reverse):
    count, place = (lax.axis_size(axis), lax.axis_index(axis))
    everything = jax.tree.map(
        lambda part, kind: lax.all_gather(part.astype(kind), axis),
        array,
        (jnp.bfloat16, jnp.bfloat16),
    )
    start = jax.tree.map(
        lambda part, zero: jnp.broadcast_to(jnp.asarray(zero, part.dtype), part.shape),
        array,
        identity,
    )

    def hop(k, before):
        at = count - 1 - k if reverse else k
        reached = at > place if reverse else at < place
        new = combine(
            before, jax.tree.map(lambda part, own: part[at].astype(own.dtype), everything, array)
        )
        return jax.tree.map(lambda a, b: jnp.where(reached, a, b), new, before)

    return lax.fori_loop(0, count, hop, start)


def modulated_norm(rows, gain, shift, scale):
    wide = rows.astype(jnp.float32)
    normed = (
        wide
        * lax.rsqrt(jnp.mean(wide * wide, axis=-1, keepdims=True) + EPS)
        * gain.astype(jnp.float32)
    )
    return (normed * (1.0 + scale) + shift).astype(jnp.bfloat16)


def project(rows, weights):
    outputs = [
        jnp.dot(rows, w, preferred_element_type=jnp.float32).astype(jnp.bfloat16) for w in weights
    ]
    return lax.optimization_barrier(outputs)


def centred_conv(padded, taps):
    wide = padded.astype(jnp.float32)
    weights = taps.astype(jnp.float32)
    length = padded.shape[0] - 2
    return jax.nn.silu(
        weights[0] * wide[:length] + weights[1] * wide[1 : length + 1] + weights[2] * wide[2:]
    )


def zero_pad(values):
    return jnp.pad(values, ((1, 1), (0, 0)))


def block_states(values, writes, step_size, decay_rate, block):
    length, heads, width = values.shape
    state = writes.shape[2]
    count = length // block
    log_decay = jnp.cumsum(-(step_size * decay_rate).reshape(count, block, heads), axis=1)
    scaled_values = (values * step_size[:, :, None]).reshape(count, block, heads, width)
    write_blocks = writes.reshape(count, block, heads, state)
    tail = jnp.exp(log_decay[:, -1:] - log_decay)
    block_sums = jnp.einsum(
        "kshn,ksh,kshp->khpn", write_blocks, tail, scaled_values, precision=lax.Precision.HIGHEST
    )
    block_decay = jnp.exp(log_decay[:, -1])

    def advance(carry, inputs):
        block_sum, decay = inputs
        return (carry * decay[:, None, None] + block_sum, carry)

    final, entering = lax.scan(
        advance, jnp.zeros((heads, width, state), jnp.float32), (block_sums, block_decay)
    )
    overall = jnp.exp(jnp.sum(log_decay[:, -1], axis=0))
    return (log_decay, scaled_values, entering, final, overall)


def block_outputs(reads, writes, log_decay, scaled_values, entering, start_state):
    count, block, heads = log_decay.shape
    state = reads.shape[2]
    read_blocks = reads.reshape(count, block, heads, state)
    write_blocks = writes.reshape(count, block, heads, state)
    starts = jnp.cumsum(log_decay[:, -1], axis=0) - log_decay[:, -1]
    entering_all = entering + jnp.exp(starts)[:, :, None, None] * start_state[None]
    forward_mask = jnp.tril(jnp.ones((block, block), bool))[None, :, :, None]
    spans = log_decay[:, :, None, :] - log_decay[:, None, :, :]
    weights = jnp.where(forward_mask, jnp.exp(jnp.where(forward_mask, spans, 0.0)), 0.0)
    intersection = jnp.einsum(
        "kqhn,kshn->kqsh", read_blocks, write_blocks, precision=lax.Precision.HIGHEST
    )
    within = jnp.einsum(
        "kqsh,kshp->kqhp", intersection * weights, scaled_values, precision=lax.Precision.HIGHEST
    )
    carried = (
        jnp.einsum("kqhn,khpn->kqhp", read_blocks, entering_all, precision=lax.Precision.HIGHEST)
        * jnp.exp(log_decay)[..., None]
    )
    return (within + carried).reshape(count * block, heads, -1)


def chain(earlier, later):
    return (earlier[0] * later[0], earlier[1] * later[0][:, None, None] + later[1])


def per_device(
    latent,
    context,
    cond,
    cond_ctx,
    mod_shift_w,
    mod_scale_w,
    mod_gate_w,
    norm_gain,
    proj_z,
    proj_x,
    proj_b,
    proj_c,
    proj_dt,
    conv_x,
    conv_b,
    conv_c,
    dt_bias,
    decay_log,
    head_gain,
    proj_out,
):
    heads = proj_x.shape[1] // HEAD_DIM
    state = proj_b.shape[1] // heads
    width_x = heads * HEAD_DIM
    width_b = heads * state
    act = jax.nn.silu(cond.astype(jnp.float32)).astype(jnp.bfloat16)
    act_ctx = jax.nn.silu(cond_ctx.astype(jnp.float32)).astype(jnp.bfloat16)
    stacked = jnp.stack([act, act_ctx])
    shift_part = jnp.dot(stacked, mod_shift_w, preferred_element_type=jnp.float32)
    scale_part = jnp.dot(stacked, mod_scale_w, preferred_element_type=jnp.float32)
    gate_part = jnp.dot(act[None], mod_gate_w, preferred_element_type=jnp.float32)
    shift_sum, scale_sum, gate_sum = lax.psum((shift_part, scale_part, gate_part), "sp")
    shifts, scales, gates = (
        lax.all_gather(shift_sum, "tp", axis=1, tiled=True),
        lax.all_gather(scale_sum, "tp", axis=1, tiled=True),
        lax.all_gather(gate_sum, "tp", axis=1, tiled=True),
    )
    normed_rows = modulated_norm(latent, norm_gain, shifts[0], scales[0])
    normed_ctx = modulated_norm(context, norm_gain, shifts[1], scales[1])
    dt_weight = lax.dynamic_slice_in_dim(proj_dt, lax.axis_index("tp") * (2 * heads), 2 * heads, 1)
    joined = jnp.concatenate(
        project(
            lax.all_gather(normed_rows, "tp", axis=0, tiled=True),
            (proj_x, proj_b, proj_c, proj_z, dt_weight),
        ),
        axis=1,
    )
    ctx_joined = lax.all_gather(
        jnp.concatenate(project(normed_ctx, (proj_x, proj_b, dt_weight)), axis=1),
        "sp",
        axis=0,
        tiled=True,
    )
    length = joined.shape[0]
    ctx_length = ctx_joined.shape[0]
    conv_end = width_x + 2 * width_b
    padded = extended(joined[:, :conv_end], (("sp", 0),), 1)
    convolved = centred_conv(padded, jnp.concatenate([conv_x, conv_b, conv_c], axis=1))
    values = convolved[:, :width_x].reshape(length, heads, HEAD_DIM)
    writes = convolved[:, width_x : width_x + width_b].reshape(length, heads, state)
    reads = convolved[:, width_x + width_b :].reshape(length, heads, state)
    z_in = joined[:, conv_end : conv_end + width_x]
    step_size = jax.nn.softplus(
        joined[:, conv_end + width_x :].astype(jnp.float32) + dt_bias
    ).reshape(length, heads, 2)
    decay_rate = jnp.exp(decay_log).reshape(heads, 2)
    ctx_conv = centred_conv(
        zero_pad(ctx_joined[:, : width_x + width_b]), jnp.concatenate([conv_x, conv_b], axis=1)
    )
    values_ctx = ctx_conv[:, :width_x].reshape(ctx_length, heads, HEAD_DIM)
    writes_ctx = ctx_conv[:, width_x:].reshape(ctx_length, heads, state)
    step_ctx = jax.nn.softplus(
        ctx_joined[:, width_x + width_b :].astype(jnp.float32) + dt_bias
    ).reshape(ctx_length, heads, 2)
    ctx_f = block_states(values_ctx, writes_ctx, step_ctx[:, :, 0], decay_rate[:, 0], BLOCK)[3]
    ctx_b = block_states(
        jnp.flip(values_ctx, 0),
        jnp.flip(writes_ctx, 0),
        jnp.flip(step_ctx[:, :, 1], 0),
        decay_rate[:, 1],
        BLOCK,
    )[3]
    log_f, scaled_f, enter_f, final_f, overall_f = block_states(
        values, writes, step_size[:, :, 0], decay_rate[:, 0], BLOCK
    )
    reads_back = jnp.flip(reads, 0)
    writes_back = jnp.flip(writes, 0)
    log_b, scaled_b, enter_b, final_b, overall_b = block_states(
        jnp.flip(values, 0), writes_back, jnp.flip(step_size[:, :, 1], 0), decay_rate[:, 1], BLOCK
    )
    identity = (jnp.ones((heads,), jnp.float32), jnp.zeros((heads, HEAD_DIM, state), jnp.float32))
    before = entering_2((overall_f, final_f), "sp", chain, identity, False)
    after = entering_2((overall_b, final_b), "sp", chain, identity, True)
    start_f = before[1] + before[0][:, None, None] * ctx_f
    start_b = after[1] + after[0][:, None, None] * ctx_b
    out_f = block_outputs(reads, writes, log_f, scaled_f, enter_f, start_f)
    out_b = block_outputs(reads_back, writes_back, log_b, scaled_b, enter_b, start_b)
    summed = out_f + jnp.flip(out_b, 0)
    gated = summed * jax.nn.silu(z_in.astype(jnp.float32)).reshape(length, heads, HEAD_DIM)
    gated = gated * lax.rsqrt(jnp.mean(gated * gated, axis=-1, keepdims=True) + EPS)
    gated = gated * head_gain.astype(jnp.float32).reshape(heads, HEAD_DIM)
    mixed_heads = gated.reshape(length, width_x).astype(jnp.bfloat16)
    update_cols = jnp.dot(
        lax.all_gather(mixed_heads, "tp", axis=1, tiled=True),
        proj_out,
        preferred_element_type=jnp.float32,
    )
    update_rows = lax.all_to_all(
        update_cols.astype(jnp.bfloat16), "tp", split_axis=0, concat_axis=1, tiled=True
    )
    update = lax.optimization_barrier(update_rows).astype(jnp.float32)
    return (latent.astype(jnp.float32) + gates[0] * update).astype(jnp.bfloat16)


MESH = pl.DeviceIdType.MESH
F32 = jnp.float32
BF16 = jnp.bfloat16


def silu(v):
    return v * (1.0 / (1.0 + jnp.exp(-v)))


def softplus(v):
    return jnp.maximum(v, 0.0) + jnp.log1p(jnp.exp(-jnp.abs(v)))


def dot_nt(a, b):
    return lax.dot_general(a, b, (((1,), (1,)), ((), ())), preferred_element_type=F32)


def dot_tn(a, b):
    return lax.dot_general(a, b, (((0,), (0,)), ((), ())), preferred_element_type=F32)


def dot_exact(a, b):
    return jnp.dot(a, b, preferred_element_type=F32, precision=lax.Precision.HIGHEST)


def iota(shape, dim):
    return lax.broadcasted_iota(jnp.int32, shape, dim)


def fused(
    sizes,
    latent_hbm,
    context_hbm,
    cond_hbm,
    cond_ctx_hbm,
    w_shift,
    w_scale,
    w_gate,
    gain_hbm,
    w_z,
    w_x,
    w_b,
    w_c,
    w_dt,
    taps_x_hbm,
    taps_b_hbm,
    taps_c_hbm,
    bias_hbm,
    decay_hbm,
    head_gain_hbm,
    w_out,
    out,
    context,
    cond,
    cond_ctx,
    gain,
    taps_x,
    taps_b,
    taps_c,
    bias_own,
    decay_own,
    head_gain,
    steps,
    mod_w,
    w_all,
    dt_w,
    out_w,
    parts,
    sums,
    raw_rows,
    h,
    proj,
    proj_d,
    ctx_x,
    ctx_b,
    ctx_d,
    edge_first,
    edge_last,
    edge_before,
    edge_after,
    taps,
    conv,
    totals,
    states_out,
    states_in,
    ctx_states,
    heads_out,
    acc,
    upd,
    upd_in,
    load_sem,
    small_sem,
    mod_send,
    mod_recv,
    sum_send,
    sum_recv,
    h_send,
    h_recv,
    m_send,
    m_recv,
    ctx_send,
    ctx_recv,
    edge_send,
    edge_recv,
    st_send,
    st_recv,
    tot_send,
    tot_recv,
    cs_send,
    cs_recv,
    up_send,
    up_recv,
):
    n_sp, n_tp, rows, ctx_rows, wx, wb, deep = sizes
    length = rows * n_tp
    ctx_len = ctx_rows * n_sp
    pairs = wx // 128
    chunk = wx
    sp = lax.axis_index("sp")
    tp = lax.axis_index("tp")
    core = tp % 2
    at_x = (tp // 2) % 2
    at_y = tp // 4

    def place(y, x, c):
        return y * 4 + x * 2 + c

    near_x = place(at_y, 1 - at_x, core)
    near_y = place(1 - at_y, at_x, core)
    mate = place(at_y, at_x, 1 - core)
    far = place(1 - at_y, 1 - at_x, core)
    mate_x = place(at_y, 1 - at_x, 1 - core)
    mate_y = place(1 - at_y, at_x, 1 - core)
    mate_far = place(1 - at_y, 1 - at_x, 1 - core)

    def sp_peer(d):
        return (sp + d) % n_sp

    def tp_peer(d):
        return (tp + d) % n_tp

    def remote(src, dst, send, recv, axis, to):
        return pltpu.make_async_remote_copy(
            src_ref=src,
            dst_ref=dst,
            send_sem=send,
            recv_sem=recv,
            device_id={axis: to},
            device_id_type=MESH,
        )

    loads = []
    mods = (w_shift, w_scale, w_gate)
    for k in range(3):
        loads.append(pltpu.make_async_copy(mods[k], mod_w.at[k], load_sem.at[k]))
    starts = (0, wx, wx + wb, wx + 2 * wb)
    for k, (src, lo, width) in enumerate(
        ((w_x, 0, wx), (w_b, wx, wb), (w_c, wx + wb, wb), (w_z, wx + 2 * wb, wx))
    ):
        loads.append(
            pltpu.make_async_copy(src, w_all.at[:, pl.ds(lo, width)], load_sem.at[3 + k])
        )
    loads.append(pltpu.make_async_copy(w_dt, dt_w, load_sem.at[7]))
    loads.append(pltpu.make_async_copy(w_out, out_w, load_sem.at[8]))
    own_rows = pl.ds(pl.multiple_of(tp * rows, rows), rows)
    small = [
        pltpu.make_async_copy(src, dst, small_sem.at[k])
        for k, (src, dst) in enumerate(
            (
                (latent_hbm, raw_rows.at[own_rows]),
                (cond_hbm, cond),
                (cond_ctx_hbm, cond_ctx),
                (context_hbm, context),
                (gain_hbm, gain),
                (taps_x_hbm, taps_x),
                (taps_b_hbm, taps_b),
                (taps_c_hbm, taps_c),
                (bias_hbm, bias_own),
                (decay_hbm, decay_own),
                (head_gain_hbm, head_gain),
            )
        )
    ]

    barrier = pltpu.get_barrier_semaphore()
    for d in range(1, n_sp):
        pl.semaphore_signal(barrier, inc=1, device_id={"sp": sp_peer(d)}, device_id_type=MESH)
    for d in range(1, n_tp):
        pl.semaphore_signal(barrier, inc=1, device_id={"tp": tp_peer(d)}, device_id_type=MESH)
    for c in small[:3]:
        c.start()
    for k in range(3):
        loads[k].start()
    for c in small[3:]:
        c.start()

    half = rows // 2

    def h_at(slot, k):
        return raw_rows.at[pl.ds(pl.multiple_of(slot * rows + k * half, half), half)]

    def m_at(slot, k):
        return heads_out.at[slot, k]

    def exchange(at, send, recv):
        plan = {
            0: (tp, 0, near_x, near_x),
            1: (tp, 1, near_x, near_x),
            2: (tp, 0, near_y, near_y),
            3: (tp, 1, near_y, near_y),
            4: (tp, 0, mate, mate),
            5: (tp, 1, mate, mate),
            6: (near_x, 0, near_y, far),
            7: (near_y, 1, near_x, far),
            8: (near_x, 0, mate, mate_x),
            9: (near_x, 1, mate, mate_x),
            10: (near_y, 0, mate, mate_y),
            11: (near_y, 1, mate, mate_y),
            12: (far, 0, mate, mate_far),
            13: (far, 1, mate, mate_far),
        }
        live = {}

        def go(k):
            slot, part, to, _ = plan[k]
            c = remote(at(slot, part), at(slot, part), send.at[k], recv.at[k], "tp", to)
            c.start()
            live[k] = c

        def got(k):
            _, part, _, slot = plan[k]
            remote(at(slot, part), at(slot, part), send.at[k], recv.at[k], "tp", mate).wait_recv()
            return slot, part

        return go, got, live

    h_go, h_got, h_live = exchange(h_at, h_send, h_recv)
    small[0].wait()
    pl.semaphore_wait(barrier, n_sp - 1 + n_tp - 1)
    for k in (0, 3, 1, 2, 4, 5):
        h_go(k)

    for c in small[1:3]:
        c.wait()
    act = silu(cond[...].astype(F32).reshape(1, -1))
    act_ctx = silu(cond_ctx[...].astype(F32).reshape(1, -1))
    row = iota((16, act.shape[1]), 0)
    stacked = jnp.where(row == 0, act, jnp.where(row == 1, act_ctx, 0.0)).astype(BF16)
    for k in range(3):
        loads[k].wait()
        if k == 2:
            for other in (3, 4, 7, 5, 6, 8):
                loads[other].start()
        part = jnp.dot(stacked, mod_w[k], preferred_element_type=F32)
        parts[sp, :, k * chunk : (k + 1) * chunk] = part[0:2]

    sends = []
    for d in range(1, n_sp):
        c = remote(parts.at[sp], parts.at[sp], mod_send.at[d], mod_recv.at[d], "sp", sp_peer(d))
        c.start()
        sends.append(c)
    for c in small[3:]:
        c.wait()
    local = 4 * pairs
    steps[...] = jnp.zeros_like(steps)
    steps[0:1, 0:local] = bias_own[...]
    steps[1:2, 0:local] = decay_own[...]
    taps[0:3, 0:wx] = taps_x[...].astype(F32)
    taps[0:3, wx : wx + wb] = taps_b[...].astype(F32)
    taps[0:3, wx + wb : wx + 2 * wb] = taps_c[...].astype(F32)
    for d in range(1, n_sp):
        sends[d - 1].wait_recv()
    total = parts[0]
    for k in range(1, n_sp):
        total = total + parts[k]
    sums[tp] = total
    for d in range(1, n_tp):
        c = remote(sums.at[tp], sums.at[tp], sum_send.at[d], sum_recv.at[d], "tp", tp_peer(d))
        c.start()
        sends.append(c)
    h_got(0)
    h_go(6)
    h_go(8)
    h_got(3)
    h_go(7)
    h_go(11)
    h_got(1)
    h_go(9)
    h_got(2)
    h_go(10)
    for d in range(1, n_tp):
        sends[n_sp - 1 + d - 1].wait_recv()

    def normed(values, which, at):
        wide = values.astype(F32)
        inv = lax.rsqrt(jnp.mean(wide * wide, axis=-1, keepdims=True) + EPS)
        for j in range(n_tp):
            lo = j * chunk
            piece = wide[:, lo : lo + chunk] * inv * gain[lo : lo + chunk].astype(F32).reshape(1, -1)
            scale = sums[j, which : which + 1, chunk : 2 * chunk]
            shift = sums[j, which : which + 1, 0:chunk]
            h[pl.ds(at, rows), lo : lo + chunk] = (piece * (1.0 + scale) + shift).astype(BF16)

    def normed_block(slot):
        at = pl.multiple_of(slot * rows, rows)
        normed(raw_rows[pl.ds(at, rows)], 0, at)

    normed_block(tp)
    for k in range(ctx_rows // rows):
        normed(context[k * rows : (k + 1) * rows], 1, length + k * rows)
    normed_block(near_x)
    normed_block(near_y)
    h_got(6)
    h_go(12)
    h_got(7)
    h_go(13)
    normed_block(far)
    for ks, slot in (((4, 5), mate), ((8, 9), mate_x), ((10, 11), mate_y), ((12, 13), mate_far)):
        for k in ks:
            h_got(k)
        normed_block(slot)

    tile = 256
    width = wx + 2 * wb
    early = wx + wb
    whole_rows = length + ctx_rows

    def project_tiles(count, lo, hi):
        def step(k, carry):
            cols = pl.ds(pl.multiple_of(k * tile, tile), tile)
            proj[0:count, cols] = jnp.dot(
                h[0:count], w_all[:, cols], preferred_element_type=F32
            ).astype(BF16)
            return carry

        lax.fori_loop(lo // tile, hi // tile, step, 0)

    edges = []

    def send_edges(lo, hi, at):
        edge_first[:, lo:hi] = proj[0:16, lo:hi].astype(F32)[0:1]
        edge_last[:, lo:hi] = proj[length - 16 : length, lo:hi].astype(F32)[15:16]
        cols = pl.ds(lo, hi - lo)
        for k, (src, dst, to) in enumerate(
            (
                (edge_last, edge_before, sp_peer(1)),
                (edge_first, edge_after, sp_peer(n_sp - 1)),
            )
        ):
            c = remote(
                src.at[:, cols],
                dst.at[:, cols],
                edge_send.at[at + k],
                edge_recv.at[at + k],
                "sp",
                to,
            )
            c.start()
            edges.append(c)

    loads[3].wait()
    loads[4].wait()
    loads[7].wait()
    project_tiles(whole_rows, 0, early)
    proj_d[...] = jnp.dot(h[...], dt_w[...], preferred_element_type=F32).astype(BF16)
    send_edges(0, early, 0)
    ctx_live = []
    for d in range(1, n_sp):
        to = sp_peer(d)
        x_cols = pl.ds(pl.multiple_of(to * 128, 128), 128)
        b_cols = pl.ds(pl.multiple_of(wx + to * 256, 128), 256)
        tail = pl.ds(length, ctx_rows)
        for k, (src, dst) in enumerate(
            (
                (proj.at[tail, x_cols], ctx_x.at[sp]),
                (proj.at[tail, b_cols], ctx_b.at[sp]),
                (proj_d.at[tail], ctx_d.at[sp]),
            )
        ):
            c = remote(src, dst, ctx_send.at[d, k], ctx_recv.at[d, k], "sp", to)
            c.start()
            ctx_live.append(c)
    ctx_x[sp] = proj[length : length + ctx_rows, pl.ds(pl.multiple_of(sp * 128, 128), 128)]
    ctx_b[sp] = proj[length : length + ctx_rows, pl.ds(pl.multiple_of(wx + sp * 256, 128), 256)]
    ctx_d[sp] = proj_d[length : length + ctx_rows]
    loads[5].wait()
    project_tiles(length, early, width)
    send_edges(early, width, 2)

    def conv_of(values, weights, before, after):
        count = values.shape[0]
        at = iota(values.shape, 0)
        prev = jnp.where(at == 0, before, pltpu.roll(values, 1, 0))
        post = jnp.where(at == count - 1, after, pltpu.roll(values, count - 1, 0))
        return silu(weights[0:1] * prev + weights[1:2] * values + weights[2:3] * post)

    bias = steps[0:1, :]
    rate = jnp.exp(steps[1:2, :])
    diag = iota((local, 128), 0) == iota((local, 128), 1)
    bias_t = jnp.sum(jnp.where(diag, bias, 0.0), axis=1, keepdims=True)
    rate_t = jnp.sum(jnp.where(diag, rate, 0.0), axis=1, keepdims=True)
    sel_row = iota((128, 128), 0)
    pick = jnp.where(
        (iota((128, 128), 1) == sel_row + local * tp) & (sel_row < local), 1.0, 0.0
    ).astype(BF16)

    def decays(raw):
        count = raw.shape[0]
        step = softplus(dot_nt(raw, pick) + bias)
        rise = -(step * rate)
        r, c = iota((count, count), 0), iota((count, count), 1)
        lower = jnp.where(c <= r, 1.0, 0.0)
        upper = jnp.where(c >= r, 1.0, 0.0)
        fwd, bwd = dot_exact(lower, rise), dot_exact(upper, rise)
        even = iota(fwd.shape, 1) % 2 == 0
        total = fwd[count - 1 : count]
        mass = jnp.exp(total - jnp.where(even, fwd, bwd)) * step
        return fwd, bwd, total, mass, lower, upper

    lane = iota((1, 128), 1)

    def pair_states(values, b_one, b_two, f_one, f_two, r_one, r_two):
        first = lane < 64
        u_f = (values * jnp.where(first, f_one, f_two)).astype(BF16)
        u_b = (values * jnp.where(first, r_one, r_two)).astype(BF16)
        f1, f2 = dot_tn(u_f, b_one), dot_tn(u_f, b_two)
        r1, r2 = dot_tn(u_b, b_one), dot_tn(u_b, b_two)
        top = iota((128, 128), 0) < 64
        return jnp.where(top, f1, f2), jnp.where(top, r1, r2)

    raw = proj_d[0:length]
    fwd, bwd, total, mass, lower, upper = decays(raw)
    totals[sp] = total
    step_t = softplus(dot_nt(pick[0:local], raw) + bias_t)
    rise_t = -(step_t * rate_t)
    fwd_t, bwd_t = dot_exact(rise_t, upper), dot_exact(rise_t, lower)
    for c in edges[:2]:
        c.wait_recv()

    def conv_tile(k, carry):
        cols = pl.ds(pl.multiple_of(k * 128, 128), 128)
        before = jnp.where(sp > 0, edge_before[:, cols], 0.0)
        after = jnp.where(sp < n_sp - 1, edge_after[:, cols], 0.0)
        conv[:, cols] = conv_of(proj[0:length, cols].astype(F32), taps[:, cols], before, after)
        return carry

    lax.fori_loop(0, early // 128, conv_tile, 0)

    def b_of(head):
        return conv[:, wx + head * 128 : wx + head * 128 + 128].astype(BF16)

    def c_of(head):
        return conv[:, wx + wb + head * 128 : wx + wb + head * 128 + 128].astype(BF16)

    for p in range(pairs):
        base = 4 * p
        cols = [mass[:, base + k : base + k + 1] for k in range(4)]
        s_f, s_b = pair_states(
            conv[:, p * 128 : p * 128 + 128],
            b_of(2 * p),
            b_of(2 * p + 1),
            cols[0],
            cols[2],
            cols[1],
            cols[3],
        )
        states_out[0, p] = s_f.astype(BF16)
        states_out[1, p] = s_b.astype(BF16)
        states_in[sp, p] = jnp.zeros((128, 128), BF16)
    st_live = []
    for d in range(1, n_sp):
        which = (sp + d) // n_sp
        c = remote(
            states_out.at[which], states_in.at[sp], st_send.at[d], st_recv.at[d], "sp", sp_peer(d)
        )
        c.start()
        st_live.append(c)
        c = remote(totals.at[sp], totals.at[sp], tot_send.at[d], tot_recv.at[d], "sp", sp_peer(d))
        c.start()
        st_live.append(c)

    for c in ctx_live:
        c.wait_recv()
    raw_ctx = ctx_d[...].reshape(ctx_len, 128)
    mass_ctx = decays(raw_ctx)[3]
    x_taps = taps[:, pl.ds(pl.multiple_of(sp * 128, 128), 128)]
    b_taps = taps[:, pl.ds(pl.multiple_of(wx + sp * 256, 128), 256)]
    xs_c = conv_of(ctx_x[...].reshape(ctx_len, 128).astype(F32), x_taps, 0.0, 0.0)
    bs_c = conv_of(ctx_b[...].reshape(ctx_len, 256).astype(F32), b_taps, 0.0, 0.0).astype(BF16)

    def column(k):
        return jnp.sum(jnp.where(lane == 4 * sp + k, mass_ctx, 0.0), axis=1, keepdims=True)

    c_f, c_b = pair_states(
        xs_c, bs_c[:, :128], bs_c[:, 128:], column(0), column(2), column(1), column(3)
    )
    ctx_states[sp, 0] = c_f.astype(BF16)
    ctx_states[sp, 1] = c_b.astype(BF16)

    cs_live = []
    for d in range(1, n_sp):
        c = remote(
            ctx_states.at[sp], ctx_states.at[sp], cs_send.at[d], cs_recv.at[d], "sp", sp_peer(d)
        )
        c.start()
        cs_live.append(c)

    loads[6].wait()
    project_tiles(length, width, width + wx)
    for c in edges[2:]:
        c.wait_recv()
    lax.fori_loop(early // 128, width // 128, conv_tile, 0)

    r, c_i = iota((length, length), 0), iota((length, length), 1)
    below, same = c_i < r, c_i == r
    first = lane < 64
    inner = []
    for p in range(pairs):
        x_p = conv[:, p * 128 : p * 128 + 128].astype(BF16)
        found = []
        for head in (2 * p, 2 * p + 1):
            f, b = 2 * head, 2 * head + 1
            score = dot_nt(c_of(head), b_of(head))
            span = jnp.where(
                below,
                fwd[:, f : f + 1] - fwd_t[f : f + 1],
                bwd[:, b : b + 1] - bwd_t[b : b + 1],
            )
            step = jnp.where(below, step_t[f : f + 1], step_t[b : b + 1]) + jnp.where(
                same, step_t[f : f + 1], 0.0
            )
            weight = (score * (jnp.exp(span) * step)).astype(BF16)
            found.append(jnp.dot(weight, x_p, preferred_element_type=F32))
        acc[:, p * 128 : p * 128 + 128] = jnp.where(first, found[0], found[1])

    for c in cs_live + st_live:
        c.wait_recv()

    m_go, m_got, m_live = exchange(m_at, m_send, m_recv)
    top = iota((128, 128), 0) < 64
    for p in range(pairs):
        base = 4 * p
        carried = []
        for way in range(2):
            state = ctx_states[p, way].astype(F32)
            for k in range(n_sp):
                q = n_sp - 1 - k if way else k
                drop = jnp.exp(
                    jnp.where(
                        top,
                        totals[q, 0:1, base + way : base + way + 1],
                        totals[q, 0:1, base + 2 + way : base + 3 + way],
                    )
                )
                reached = q > sp if way else q < sp
                state = jnp.where(reached, state * drop + states_in[q, p].astype(F32), state)
            start = state.astype(BF16)
            one, two = dot_nt(c_of(2 * p), start), dot_nt(c_of(2 * p + 1), start)
            log = bwd if way else fwd
            fade = jnp.exp(
                jnp.where(
                    first,
                    log[:, base + way : base + way + 1],
                    log[:, base + 2 + way : base + 3 + way],
                )
            )
            carried.append(jnp.where(first, one, two) * fade)
        cols = slice(p * 128, p * 128 + 128)
        z_in = proj[0:length, width + p * 128 : width + p * 128 + 128].astype(F32)
        g = (acc[:, cols] + carried[0] + carried[1]) * silu(z_in)
        square = g * g
        mean_1 = jnp.sum(jnp.where(first, square, 0.0), axis=1, keepdims=True) / 64.0
        mean_2 = jnp.sum(jnp.where(first, 0.0, square), axis=1, keepdims=True) / 64.0
        inv = jnp.where(first, lax.rsqrt(mean_1 + EPS), lax.rsqrt(mean_2 + EPS))
        done = (g * inv * head_gain[cols].astype(F32).reshape(1, -1)).astype(BF16)
        per = pairs // 2
        heads_out[tp, p // per, :, (p % per) * 128 : (p % per) * 128 + 128] = done
        if p % per == per - 1:
            for k in ((0, 2, 4) if p // per == 0 else (3, 1, 5)):
                m_go(k)

    loads[8].wait()
    piece = wx // 2

    def gather_add(slot, k, fresh=False):
        at = pl.ds(pl.multiple_of(slot * wx + k * piece, piece), piece)
        new = jnp.dot(heads_out[slot, k], out_w[at, :], preferred_element_type=F32)
        acc[...] = new if fresh else acc[...] + new

    gather_add(tp, 0, True)
    gather_add(tp, 1)
    a = m_got(0)
    m_go(6)
    m_go(8)
    gather_add(*a)
    gather_add(*m_got(4))
    a = m_got(3)
    m_go(7)
    m_go(11)
    gather_add(*a)
    a = m_got(1)
    m_go(9)
    b = m_got(2)
    m_go(10)
    gather_add(*a)
    gather_add(*b)
    for k in (5, 8):
        gather_add(*m_got(k))
    a = m_got(6)
    m_go(12)
    b = m_got(7)
    m_go(13)
    gather_add(*a)
    gather_add(*b)
    for k in (11, 9, 10, 12, 13):
        gather_add(*m_got(k))

    upd[...] = acc[...].astype(BF16)
    up_live = []
    for d in range(1, n_tp):
        to = tp_peer(d)
        src = upd.at[pl.ds(pl.multiple_of(to * rows, rows), rows)]
        c = remote(src, upd_in.at[tp], up_send.at[d], up_recv.at[d], "tp", to)
        c.start()
        up_live.append(c)
    upd_in[tp] = upd[pl.ds(pl.multiple_of(tp * rows, rows), rows)]
    for c in up_live:
        c.wait_recv()
    for j in range(n_tp):
        cols = slice(j * chunk, (j + 1) * chunk)
        gate = sums[j, 0:1, 2 * chunk : 3 * chunk]
        out[:, cols] = (raw_rows[own_rows, cols].astype(F32) + gate * upd_in[j].astype(F32)).astype(BF16)
    for c in (
        sends
        + list(h_live.values())
        + ctx_live
        + cs_live
        + edges
        + st_live
        + list(m_live.values())
        + up_live
    ):
        c.wait_send()


def per_device_fused(
    n_sp,
    n_tp,
    latent,
    context,
    cond,
    cond_ctx,
    mod_shift_w,
    mod_scale_w,
    mod_gate_w,
    norm_gain,
    proj_z,
    proj_x,
    proj_b,
    proj_c,
    proj_dt,
    conv_x,
    conv_b,
    conv_c,
    dt_bias,
    decay_log,
    head_gain,
    proj_out,
):
    rows, deep = latent.shape
    ctx_rows = context.shape[0]
    wx, wb = proj_x.shape[1], proj_b.shape[1]
    length, pairs = rows * n_tp, wx // 128
    width = wx + 2 * wb
    bias, decay = dt_bias[None], decay_log[None]
    vmem = pl.BlockSpec(memory_space=pltpu.VMEM)
    hbm = pl.BlockSpec(memory_space=pltpu.HBM)
    dma = pltpu.SemaphoreType.DMA
    small = (
        context, cond, cond_ctx, norm_gain, conv_x, conv_b, conv_c, bias, decay, head_gain,
    )
    scratch = [pltpu.VMEM(a.shape, a.dtype) for a in small] + [
        pltpu.VMEM((8, 128), F32),
        pltpu.VMEM((3,) + mod_shift_w.shape, BF16),
        pltpu.VMEM((deep, width + wx), BF16),
        pltpu.VMEM(proj_dt.shape, BF16),
        pltpu.VMEM(proj_out.shape, BF16),
        pltpu.VMEM((n_sp, 2, 3 * wx), F32),
        pltpu.VMEM((n_tp, 2, 3 * wx), F32),
        pltpu.VMEM((length, deep), BF16),
        pltpu.VMEM((length + ctx_rows, deep), BF16),
        pltpu.VMEM((length + ctx_rows, width + wx), BF16),
        pltpu.VMEM((length + ctx_rows, 128), BF16),
        pltpu.VMEM((n_sp, ctx_rows, 128), BF16),
        pltpu.VMEM((n_sp, ctx_rows, 256), BF16),
        pltpu.VMEM((n_sp, ctx_rows, 128), BF16),
        pltpu.VMEM((1, width), F32),
        pltpu.VMEM((1, width), F32),
        pltpu.VMEM((1, width), F32),
        pltpu.VMEM((1, width), F32),
        pltpu.VMEM((8, width), F32),
        pltpu.VMEM((length, width), F32),
        pltpu.VMEM((n_sp, 1, 128), F32),
        pltpu.VMEM((2, pairs, 128, 128), BF16),
        pltpu.VMEM((n_sp, pairs, 128, 128), BF16),
        pltpu.VMEM((n_sp, 2, 128, 128), BF16),
        pltpu.VMEM((n_tp, 2, length, wx // 2), BF16),
        pltpu.VMEM((length, wx), F32),
        pltpu.VMEM((length, wx), BF16),
        pltpu.VMEM((n_tp, rows, wx), BF16),
        dma((9,)),
        dma((11,)),
    ]
    for shape in (
        (n_sp,), (n_tp,), (14,), (14,), (n_sp, 3), (4,), (n_sp,), (n_sp,), (n_sp,), (n_tp,)
    ):
        scratch += [dma(shape), dma(shape)]
    return pl.pallas_call(
        functools.partial(fused, (n_sp, n_tp, rows, ctx_rows, wx, wb, deep)),
        out_shape=pltpu.VMEM(latent.shape, BF16),
        in_specs=[hbm] * 20,
        out_specs=vmem,
        scratch_shapes=scratch,
        compiler_params=pltpu.CompilerParams(
            collective_id=0, has_side_effects=True, vmem_limit_bytes=60 * 1024 * 1024
        ),
    )(
        latent, context, cond, cond_ctx, mod_shift_w, mod_scale_w, mod_gate_w,
        norm_gain, proj_z, proj_x, proj_b, proj_c, proj_dt, conv_x, conv_b, conv_c,
        bias, decay, head_gain, proj_out,
    )


def fits(mesh, latent, context, proj_x, proj_b, proj_dt):
    n_sp, n_tp = mesh.shape["sp"], mesh.shape["tp"]
    heads = proj_x.shape[1] // HEAD_DIM // n_tp
    rows, ctx_rows = latent.shape[0] // (n_sp * n_tp), context.shape[0] // n_sp
    return (
        n_tp == 8
        and heads == 2 * n_sp
        and heads % 4 == 0
        and proj_b.shape[1] == 2 * proj_x.shape[1]
        and proj_x.shape[1] == latent.shape[1]
        and proj_dt.shape[1] == 128
        and rows % 32 == 0
        and ctx_rows % rows == 0
    )


def solution(mesh):
    placed = (
        P(("sp", "tp"), None),
        P("sp", None),
        P("sp"),
        P("sp"),
        P("sp", "tp"),
        P("sp", "tp"),
        P("sp", "tp"),
        P(),
        P(None, "tp"),
        P(None, "tp"),
        P(None, "tp"),
        P(None, "tp"),
        P(),
        P(None, "tp"),
        P(None, "tp"),
        P(None, "tp"),
        P("tp"),
        P("tp"),
        P("tp"),
        P(None, "tp"),
    )
    def place(body):
        return jax.shard_map(
            body, mesh=mesh, in_specs=placed, out_specs=P(("sp", "tp"), None), check_vma=False
        )

    def step(*arrays):
        latent, context, proj_x, proj_b, proj_dt = (arrays[k] for k in (0, 1, 9, 10, 12))
        if fits(mesh, latent, context, proj_x, proj_b, proj_dt):
            return place(
                functools.partial(per_device_fused, mesh.shape["sp"], mesh.shape["tp"])
            )(*arrays)
        return place(per_device)(*arrays)

    return step
```
